32 devices in a mesh: ep: 8 (over z, x), tp: 4 (over y, core).
Axes of the slice: x: 2, y: 2, z: 4, core: 2. Of those that a mesh axis runs over, the one named last changes fastest.
Arguments:
- queries: bfloat16 [4096, 1024], P('ep', 'tp'), may hold values from -6 to 6
- forget_forward_logits: bfloat16 [4096, 1024], P('ep', 'tp'), may hold values from -6 to 12
- forget_backward_logits: bfloat16 [4096, 1024], P('ep', 'tp'), may hold values from -6 to 12
- values: bfloat16 [4096, 1024], P('ep', 'tp'), may hold values from -6 to 6
- output_gate_logits: bfloat16 [4096, 1024], P('ep', 'tp'), may hold values from -6 to 6
- lower_bound_forward: float32 [1024], P('tp')
- lower_bound_backward: float32 [1024], P('tp')
- extra_log_decay: float32 [4096, 8], P('ep', 'tp'), may hold values from -2 to 0
- head_norm_scale: float32 [1024], P('tp'), may hold values from 0.1 to 1.9
- output_projection: bfloat16 [1024, 2048], P('tp'), may hold values from -0.1875 to 0.1875
- second_residual: bfloat16 [4096, 2048], P('ep'), may hold values from -6 to 6
- expert_norm_scale: float32 [2048], replicated, may hold values from 0.1 to 1.9
- routes: int32 [4096, 2], P('ep'), may hold values from 0 to 7, all different within a row; in each aligned block of 128 rows (0 to 127, 128 to 255, ...) at most 64 rows name the same one
- specialist_mixing_factor: float32 [4096, 2], P(('ep', 'tp')), may hold values from 0.1 to 1
- expert_gate_matrix: bfloat16 [8, 2048, 1024], P('ep', None, 'tp'), may hold values from -0.125 to 0.125
- expert_up_matrix: bfloat16 [8, 2048, 1024], P('ep', None, 'tp'), may hold values from -0.125 to 0.125
- expert_down_matrix: bfloat16 [8, 1024, 2048], P('ep', 'tp'), may hold values from -0.1875 to 0.1875
Outputs:
- mixer_output: bfloat16 [4096, 2048], P(('ep', 'tp'))
- routed_output: bfloat16 [4096, 2048], P(('ep', 'tp'))
The draws below stay inside these ranges and needn't reach their ends.
Inputs may be any that keep to these rules, and one draw needn't show every extreme that they name: `routes`: in each aligned block of 128 rows no expert is named by more than 64 rows; the 2 experts of a row differ.
All inputs are finite; a program needn't handle non-finite values.
Results may differ from the reference program's by a relative error of at most 0.014.
Values may be sent and summed in bfloat16 or wider, within the bound.
A program may use at most 128 MiB of HBM per device.

```python
import math
import jax
import jax.numpy as jnp
import numpy as np
from jax import lax

D = 2048
RECURRENT_HEADS = 8
DK = 128
DV = 128
FF = 1024
TOPK = 2
SPAN = 64
ROWS = 128
KEY_WIDTH = 1024
VAL_WIDTH = 1024
GROUP_WIDTH = 256
EXPERT_PART = 256
EXPERTS = 8
CAPQ = 64
TOKENS_A = 4096
TOKENS_B = 4096
N_EP = 8
N_TP = 4


def floor_common(key, salt):
    key = jax.random.fold_in(key, salt)
    key_order, key_slow, key_fast = jax.random.split(key, 3)
    ordering = jax.random.permutation(key_order, RECURRENT_HEADS)
    slow_heads = ordering < RECURRENT_HEADS // 2
    slow_rate = jax.random.uniform(key_slow, (RECURRENT_HEADS, DK), jnp.float32, 0.3, 2.0) / TOKENS_A
    fast_rate = jnp.exp(jax.random.uniform(key_fast, (RECURRENT_HEADS, DK), jnp.float32, math.log(0.025), math.log(0.1)))
    decay_rate = jnp.where(slow_heads[:, None], slow_rate, fast_rate)
    return (jnp.log1p(-decay_rate) - jnp.log(decay_rate)).reshape(RECURRENT_HEADS * DK).astype(jnp.float32)


def draw_lower_bound_forward(key, part):
    return floor_common(key, 11)


def draw_lower_bound_backward(key, part):
    return floor_common(key, 12)


def forget_common(key, salt):
    key = jax.random.fold_in(key, salt)
    key_base, key_run = jax.random.split(key, 2)
    base = jnp.clip(1.5 * jax.random.normal(key_base, (TOKENS_A, RECURRENT_HEADS, DK), jnp.float32), -6.0, 6.0)
    run_length = 4 * SPAN
    run_count = (TOKENS_A + run_length - 1) // run_length
    lifted = 6.0 * jax.random.randint(key_run, (run_count, RECURRENT_HEADS), 0, 2).astype(jnp.float32)
    position_block = jnp.arange(TOKENS_A, dtype=jnp.int32) // run_length
    offsets = lifted[position_block]
    return (base + offsets[:, :, None]).reshape(TOKENS_A, RECURRENT_HEADS * DK).astype(jnp.float32)


def draw_forget_forward_logits(key, part):
    return forget_common(key, 21).astype(jnp.bfloat16)


def draw_forget_backward_logits(key, part):
    return forget_common(key, 22).astype(jnp.bfloat16)


def draw_extra_log_decay(key, part):
    key_rate, key_place, key_depth = jax.random.split(key, 3)
    span_rows = TOKENS_A // EXPERTS
    factor = jnp.exp(jax.random.uniform(key_rate, (EXPERTS, RECURRENT_HEADS), jnp.float32, 0.0, math.log(3.0)))
    token_position = jnp.arange(TOKENS_A, dtype=jnp.int32)
    owner_block = token_position // span_rows
    stable_state = -0.2 / TOKENS_A * factor[owner_block]
    slot_positions = jax.random.randint(key_place, (2, RECURRENT_HEADS), 0, TOKENS_A)
    cumulative_decay = jnp.log(jax.random.uniform(key_depth, (2, RECURRENT_HEADS), jnp.float32, 0.55, 0.8))
    extra_decay_hits = token_position[:, None, None] == slot_positions[None, :, :]
    return (stable_state + jnp.sum(jnp.where(extra_decay_hits, cumulative_decay[None], 0.0), axis=1)).astype(jnp.float32)


def shard_levels(key, shape, cuts, low, high):
    level, own = 1.0, jax.random.fold_in(key, 6)
    for position, shards_of in cuts:
        draws = jnp.exp(jax.random.uniform(jax.random.fold_in(own, position), (shards_of,), jnp.float32, low / len(cuts), high / len(cuts)))
        level = level * jnp.repeat(draws, shape[position] // shards_of).reshape([-1 if axis == position else 1 for axis in range(len(shape))])
    return level


def deal_out(own_key, own, number, rows, count, top, most, lean):
    ranking = jax.random.permutation(own_key, count)
    crowded, common = load_shares(count, rows * top, most, lean, True), load_shares(count, rows * top, most, lean, False)
    places = jnp.arange(count)

    def named(sizes, offset_by):
        used = int((sizes > 0).sum())
        fixed = max(1, used // 4)
        passed = fixed + (places - fixed + offset_by * (used - fixed)) % max(1, count - fixed)
        return jnp.zeros((count,), jnp.int32).at[ranking[jnp.where(places < fixed, places, passed)]].set(jnp.asarray(sizes, jnp.int32))

    sizes = jnp.where(number % 4 == 0, named(crowded, number // 4), named(common, number - number // 4 - 1))
    mixed = jax.random.permutation(jax.random.fold_in(own, 3), count)
    source_of, receiver = mixed[0:count // 2 * 2:2], mixed[1:count // 2 * 2:2]
    slack = jnp.minimum(sizes[source_of] - 1, most - sizes[receiver]) // 2
    slack = jnp.where((source_of == ranking[0]) | (receiver == ranking[0]) | (sizes[receiver] == 0), 0, jnp.maximum(slack, 0))
    passed = jax.random.randint(jax.random.fold_in(own, 4), (count // 2,), 0, 1 << 20) % (slack + 1)
    sizes = sizes.at[source_of].add(-passed).at[receiver].add(passed)
    members = jnp.searchsorted(jnp.cumsum(sizes), jnp.arange(rows * top), side="right").astype(jnp.int32)
    table = members.reshape(top, rows).T
    table = table[jax.random.permutation(jax.random.fold_in(own, 1), rows)]
    offset_by = jax.random.randint(jax.random.fold_in(own, 2), (rows, 1), 0, top)
    return jnp.take_along_axis(table, (jnp.arange(top)[None, :] + offset_by) % top, axis=1)


def load_shares(count, total, bound, skew, full):
    weights = [(1 << 20) // math.isqrt(standing ** skew) + 1 for standing in range(1, count + 1)]
    largest = bound if full else min(bound, max(-(-total // count), total * weights[0] // sum(weights)))
    least = 1 if total - largest >= count - 1 else 0
    given, rest = [largest] + [least] * (count - 1), total - largest - least * (count - 1)
    while rest > 0:
        movable = [i for i in range(1, count) if given[i] < largest] or [i for i in range(1, count) if given[i] < bound]
        mass, remaining = sum([weights[i] for i in movable]), rest
        for i in movable:
            extra = min(bound - given[i], max(1, remaining * weights[i] // mass), rest)
            given[i] = given[i] + extra
            rest = rest - extra
    return np.array(given)


def noise(stream_key, shape, deviation, bound, shards=(), held_as=jnp.bfloat16):
    loudness = shard_levels(stream_key, shape, shards, -0.22, 0.18) if shards else 1.0
    entries = jax.random.normal(stream_key, shape, jnp.float32) * deviation * loudness
    return jnp.minimum(jnp.maximum(entries, -bound), bound).astype(held_as)


def setup_inputs(seed: int = 0) -> dict:
    arg_keys = jax.random.split(jax.random.key(seed), 18)
    queries = noise(arg_keys[0], (TOKENS_A, KEY_WIDTH), 1.0, 6.0, ((0, 8), (1, 4)))
    forget_forward_logits = draw_forget_forward_logits(jax.random.fold_in(arg_keys[17], 71), 0)
    forget_backward_logits = draw_forget_backward_logits(jax.random.fold_in(arg_keys[17], 71), 0)
    values = noise(arg_keys[3], (TOKENS_A, VAL_WIDTH), 1.0, 6.0, ((0, 8), (1, 4)))
    output_gate_logits = noise(arg_keys[4], (TOKENS_A, VAL_WIDTH), 1.0, 6.0, ((0, 8), (1, 4)))
    lower_bound_forward = draw_lower_bound_forward(jax.random.fold_in(arg_keys[17], 71), 0)
    lower_bound_backward = draw_lower_bound_backward(jax.random.fold_in(arg_keys[17], 71), 0)
    extra_log_decay = draw_extra_log_decay(jax.random.fold_in(arg_keys[17], 71), 0)
    head_norm_scale = jnp.clip(1.0 + 0.18 * jax.random.normal(arg_keys[8], (VAL_WIDTH,), jnp.float32), 0.1, 1.9)
    output_projection = noise(arg_keys[9], (VAL_WIDTH, D), VAL_WIDTH ** -0.5, 0.1875, ((0, 4),))
    second_residual = noise(arg_keys[10], (TOKENS_B, D), 1.0, 6.0, ((0, 8),))
    expert_norm_scale = jnp.clip(1.0 + 0.18 * jax.random.normal(arg_keys[11], (D,), jnp.float32), 0.1, 1.9)
    routes_keys = jax.random.split(jax.random.fold_in(arg_keys[12], 1), TOKENS_B // ROWS)
    routes_turns = jax.random.permutation(jax.random.fold_in(arg_keys[12], 3), TOKENS_B // ROWS)
    routes = jax.vmap(lambda own, number: deal_out(jax.random.fold_in(arg_keys[12], 2), own, number, ROWS, EXPERTS, TOPK, CAPQ, 2))(routes_keys, routes_turns).reshape((TOKENS_B, TOPK))
    specialist_mixing_factor = jnp.clip(0.1 + 0.9 * jax.random.uniform(arg_keys[13], (TOKENS_B, TOPK), jnp.float32) ** shard_levels(arg_keys[13], (TOKENS_B, TOPK), ((0, 32),), -0.2, 0.2), 0.1, 1.0)
    expert_gate_matrix = noise(arg_keys[14], (EXPERTS, D, FF), D ** -0.5, 0.125, ((0, 8), (2, 4)))
    expert_up_matrix = noise(arg_keys[15], (EXPERTS, D, FF), D ** -0.5, 0.125, ((0, 8), (2, 4)))
    expert_down_matrix = noise(arg_keys[16], (EXPERTS, FF, D), FF ** -0.5, 0.1875, ((0, 8), (1, 4)))
    return dict(queries=queries, forget_forward_logits=forget_forward_logits, forget_backward_logits=forget_backward_logits, values=values, output_gate_logits=output_gate_logits, lower_bound_forward=lower_bound_forward, lower_bound_backward=lower_bound_backward, extra_log_decay=extra_log_decay, head_norm_scale=head_norm_scale, output_projection=output_projection, second_residual=second_residual, expert_norm_scale=expert_norm_scale, routes=routes, specialist_mixing_factor=specialist_mixing_factor, expert_gate_matrix=expert_gate_matrix, expert_up_matrix=expert_up_matrix, expert_down_matrix=expert_down_matrix)


EPS = 1e-06
PRECISE_PRODUCT = lax.Precision.HIGHEST

def block_pass(feature, key_matrix_rows, value_rows, log_forget_decay):
    row_count, number_of_heads, channels = feature.shape
    blocks = row_count // SPAN
    lower_mask = jnp.tril(jnp.ones((SPAN, SPAN), bool))[:, :, None, None]

    def shaped(tensor):
        return tensor.reshape(blocks, SPAN, number_of_heads, tensor.shape[-1])

    def advance(progress, inputs):
        recurrent_memory, offset = progress
        query_tile_rows, address_piece_entries, content_piece_entries, decay_block = inputs
        progressive_summary = jnp.cumsum(decay_block, axis=0)
        spread_log = jnp.where(lower_mask, progressive_summary[:, None] - progressive_summary[None, :], -jnp.inf)
        scores = lax.optimization_barrier(jnp.sum(query_tile_rows[:, None] * address_piece_entries[None, :] * jnp.exp(spread_log), axis=-1))
        inner_part = jnp.einsum('tsh,shv->thv', scores, content_piece_entries, precision=PRECISE_PRODUCT)
        handed_summary = jnp.einsum('wbf,bfl->wbl', query_tile_rows * jnp.exp(progressive_summary), recurrent_memory, precision=PRECISE_PRODUCT)
        segment_fading_total = progressive_summary[-1]
        trained_portion = jnp.einsum('gkf,gkr->kfr', address_piece_entries * jnp.exp(segment_fading_total[None] - progressive_summary), content_piece_entries, precision=PRECISE_PRODUCT)
        recurrent_memory = jnp.exp(segment_fading_total)[:, :, None] * recurrent_memory + trained_portion
        return ((recurrent_memory, offset + segment_fading_total), (inner_part + handed_summary, query_tile_rows * jnp.exp(progressive_summary + offset)))
    initial = (jnp.zeros((number_of_heads, channels, value_rows.shape[-1]), jnp.float32), jnp.zeros((number_of_heads, channels), jnp.float32))
    (recurrent_memory, decay_total), (output_rows, query_decay_reach) = lax.scan(advance, initial, (shaped(feature), shaped(key_matrix_rows), shaped(value_rows), shaped(log_forget_decay)))
    return (output_rows.reshape(row_count, number_of_heads, -1), query_decay_reach.reshape(row_count, number_of_heads, channels), recurrent_memory, decay_total)

def forget_gate_terms(forget_gate_input, lower_bound_logit, extra_decay_rows, number_of_heads):
    row_count = forget_gate_input.shape[0]
    widened_values = forget_gate_input.astype(jnp.float32).reshape(row_count, number_of_heads, -1)
    lower_bound_share = jax.nn.sigmoid(lower_bound_logit).reshape(number_of_heads, -1)
    remaining_fraction = jax.nn.sigmoid(-lower_bound_logit).reshape(number_of_heads, -1)
    log_forget_decay = jnp.log(lower_bound_share + remaining_fraction * jax.nn.sigmoid(widened_values)) + extra_decay_rows[:, :, None]
    return (remaining_fraction * jax.nn.sigmoid(-widened_values), log_forget_decay)

def finish_heads(combined, head_norm_scale, output_gate_logits, number_of_heads):
    mean_square = lax.optimization_barrier(jnp.mean(combined * combined, axis=-1, keepdims=True))
    scaled = combined * lax.rsqrt(mean_square + EPS) * head_norm_scale.reshape(number_of_heads, -1)
    opened = scaled * jax.nn.silu(output_gate_logits.astype(jnp.float32)).reshape(combined.shape)
    return opened.astype(jnp.bfloat16).reshape(combined.shape[0], -1)

def normalize(tensor, gain):
    widened_values = tensor.astype(jnp.float32)
    return (widened_values * lax.rsqrt(lax.optimization_barrier(jnp.mean(widened_values * widened_values, axis=-1, keepdims=True)) + EPS) * gain).astype(jnp.bfloat16)

def reference(queries, forget_forward_logits, forget_backward_logits, values, output_gate_logits, lower_bound_forward, lower_bound_backward, extra_log_decay, head_norm_scale, output_projection, second_residual, expert_norm_scale, routes, specialist_mixing_factor, expert_gate_matrix, expert_up_matrix, expert_down_matrix):
    feature = jax.nn.silu(queries.astype(jnp.float32)).reshape(TOKENS_A, RECURRENT_HEADS, DK)
    value_rows = values.astype(jnp.float32).reshape(TOKENS_A, RECURRENT_HEADS, DV)
    combined = jnp.zeros(value_rows.shape, jnp.float32)
    for forget_gate_input, lower_bound_logit, reverse in ((forget_forward_logits, lower_bound_forward, False), (forget_backward_logits, lower_bound_backward, True)):
        key_matrix_rows, log_forget_decay = forget_gate_terms(forget_gate_input, lower_bound_logit, extra_log_decay, RECURRENT_HEADS)
        if reverse:
            output_rows = block_pass(jnp.flip(feature, 0), jnp.flip(key_matrix_rows, 0), jnp.flip(value_rows, 0), jnp.flip(log_forget_decay, 0))[0]
            output_rows = jnp.flip(output_rows, 0)
        else:
            output_rows = block_pass(feature, key_matrix_rows, value_rows, log_forget_decay)[0]
        combined = combined + output_rows
    mixer_hidden = finish_heads(combined, head_norm_scale, output_gate_logits, RECURRENT_HEADS)
    summed = jnp.zeros((TOKENS_A, D), jnp.float32)
    for group_index in range(N_TP):
        lower_edge = group_index * GROUP_WIDTH
        partial_value = jnp.dot(mixer_hidden[:, lower_edge:lower_edge + GROUP_WIDTH], output_projection[lower_edge:lower_edge + GROUP_WIDTH], preferred_element_type=jnp.float32)
        summed = summed + lax.optimization_barrier(partial_value.astype(jnp.bfloat16)).astype(jnp.float32)
    mixer_output = summed.astype(jnp.bfloat16)
    routed_normed = normalize(second_residual, expert_norm_scale)
    slot_total = N_EP * N_TP * CAPQ
    token_ids = jnp.arange(TOKENS_B, dtype=jnp.int32)

    def one_expert(accumulated, expert):
        chosen = routes == expert
        weight = lax.optimization_barrier(jnp.sum(jnp.where(chosen, specialist_mixing_factor, 0.0), axis=1))
        member = jnp.any(chosen, axis=1)
        token_position = (jnp.cumsum(member.astype(jnp.int32)) - 1).astype(jnp.int32)
        token_position = jnp.where(member, token_position, slot_total).astype(jnp.int32)
        slot_table = jnp.zeros((slot_total + 1,), jnp.int32).at[token_position].set(token_ids)[:slot_total]
        slot_weight = jnp.zeros((slot_total + 1,), jnp.float32).at[token_position].set(weight)[:slot_total]
        picked = routed_normed[slot_table]
        gated = jnp.dot(picked, expert_gate_matrix[expert], preferred_element_type=jnp.float32)
        lifted = jnp.dot(picked, expert_up_matrix[expert], preferred_element_type=jnp.float32)
        expert_hidden = (jax.nn.silu(gated) * lifted).astype(jnp.bfloat16)
        down_rows = expert_down_matrix[expert]
        result = jnp.zeros((slot_total, D), jnp.float32)
        for group_index in range(N_TP):
            lower_edge = group_index * EXPERT_PART
            partial_value = jnp.dot(expert_hidden[:, lower_edge:lower_edge + EXPERT_PART], down_rows[lower_edge:lower_edge + EXPERT_PART], preferred_element_type=jnp.float32)
            result = result + lax.optimization_barrier(partial_value.astype(jnp.bfloat16)).astype(jnp.float32)
        expert_result = lax.optimization_barrier(result.astype(jnp.bfloat16)).astype(jnp.float32)
        accumulated = accumulated.at[slot_table].add(slot_weight[:, None] * expert_result)
        return (accumulated, None)
    accumulated = lax.scan(one_expert, jnp.zeros((TOKENS_B, D), jnp.float32), jnp.arange(EXPERTS, dtype=jnp.int32))[0]
    routed_output = accumulated.astype(jnp.bfloat16)
    return (mixer_output, routed_output)
```

```python
import functools

import jax
import jax.numpy as jnp
from jax import lax
from jax.experimental import pallas as pl
from jax.experimental.pallas import tpu as pltpu
from jax.sharding import PartitionSpec as P

TOPK = 2
CHUNK = 128
LEAF = 16
DECAY_ROWS = 16
EPS = 1e-06
MESH = pl.DeviceIdType.MESH
F32 = jnp.float32
BF16 = jnp.bfloat16


def greet(n):
    me = lax.axis_index("ep")
    barrier = pltpu.get_barrier_semaphore()

    def one(step, carry):
        peer = lax.rem(me + step, n)
        pl.semaphore_signal(barrier, inc=1, device_id={"ep": peer}, device_id_type=MESH)
        return carry

    lax.fori_loop(1, n, one, 0)
    pl.semaphore_wait(barrier, n - 1)


def block_copy(out_ref, in_ref, send_sem, recv_sem, target, source):
    me = lax.axis_index("ep")
    return pltpu.make_async_remote_copy(
        src_ref=out_ref.at[target],
        dst_ref=in_ref.at[source],
        send_sem=send_sem.at[target],
        recv_sem=recv_sem.at[source],
        device_id={"ep": target},
        device_id_type=MESH,
    )


def start_blocks(n, out_ref, in_ref, send_sem, recv_sem):
    me = lax.axis_index("ep")

    def one(step, carry):
        peer = lax.rem(me + step, n)
        block_copy(out_ref, in_ref, send_sem, recv_sem, peer, me).start()
        return carry

    lax.fori_loop(1, n, one, 0)
    in_ref[me] = out_ref[me]


def finish_blocks(n, out_ref, in_ref, send_sem, recv_sem):
    me = lax.axis_index("ep")

    def one(step, carry):
        peer = lax.rem(me + step, n)
        copy = block_copy(out_ref, in_ref, send_sem, recv_sem, peer, peer)
        copy.wait_send()
        copy.wait_recv()
        return carry

    lax.fori_loop(1, n, one, 0)


def exchange_kernel(n, out_ref, in_ref, send_sem, recv_sem):
    greet(n)
    start_blocks(n, out_ref, in_ref, send_sem, recv_sem)
    finish_blocks(n, out_ref, in_ref, send_sem, recv_sem)


def exchange(blocks, n):
    vmem = pl.BlockSpec(memory_space=pltpu.VMEM)
    return pl.pallas_call(
        functools.partial(exchange_kernel, n),
        out_shape=jax.ShapeDtypeStruct(blocks.shape, blocks.dtype),
        in_specs=[vmem],
        out_specs=vmem,
        scratch_shapes=[pltpu.SemaphoreType.DMA((n,)), pltpu.SemaphoreType.DMA((n,))],
        compiler_params=pltpu.CompilerParams(collective_id=1, has_side_effects=True),
        cost_estimate=pl.CostEstimate(
            flops=2 * 10**10, bytes_accessed=2 * blocks.size * 2, transcendentals=0
        ),
        name="return_rows",
    )(blocks)


def dot_rows(a, b):
    return lax.dot_general(a, b, (((1,), (1,)), ((), ())), preferred_element_type=F32)


def gates(logits, bound, extra):
    shrink = jnp.exp(-logits)
    opened = 1.0 / (1.0 + shrink)
    floor_part = 1.0 / (1.0 + jnp.exp(-bound))
    complement = 1.0 / (1.0 + jnp.exp(bound))
    decay = jnp.log(floor_part + complement * opened) + extra
    return complement * (shrink * opened), decay


def referenced(total, size, place):
    blocks = total.reshape(CHUNK // size, size, total.shape[-1])
    anchor = jnp.broadcast_to(blocks[:, place : place + 1, :], blocks.shape)
    return total - anchor.reshape(total.shape)


def chunk_scores(feature, key, total, backward, rows, cols):
    scores = jnp.zeros((CHUNK, CHUNK), F32)
    size = CHUNK
    while size > LEAF:
        half = size // 2
        reach = jnp.exp(-jnp.abs(referenced(total, size, half if backward else half - 1)))
        part = dot_rows((feature * reach).astype(BF16), (key * reach).astype(BF16))
        late, early = (cols, rows) if backward else (rows, cols)
        mask = (rows // size == cols // size) & (late % size >= half) & (early % size < half)
        scores = scores + jnp.where(mask, part, 0.0)
        size = half
    spread = referenced(total, LEAF, LEAF // 2 if backward else LEAF // 2 - 1)
    part = dot_rows(
        (feature * jnp.exp(spread)).astype(BF16), (key * jnp.exp(-spread)).astype(BF16)
    )
    mask = (rows // LEAF == cols // LEAF) & ((rows <= cols) if backward else (rows >= cols))
    return scores + jnp.where(mask, part, 0.0)


def mixer_kernel(
    n,
    q_ref,
    ff_ref,
    fb_ref,
    v_ref,
    og_ref,
    lbf_ref,
    lbb_ref,
    extra_ref,
    scale_ref,
    slots_ref,
    hidden_ref,
    arrived_ref,
    local_ref,
    reach_ref,
    part_ref,
    fade_ref,
    state_out,
    state_in,
    slot_send,
    slot_recv,
    state_send,
    state_recv,
):
    me = lax.axis_index("ep")
    row_count, width = q_ref.shape
    chunks = row_count // CHUNK
    heads = extra_ref.shape[1]
    channels = width // heads
    greet(n)
    start_blocks(n, slots_ref, arrived_ref, slot_send, slot_recv)
    rows = lax.broadcasted_iota(jnp.int32, (CHUNK, CHUNK), 0)
    cols = lax.broadcasted_iota(jnp.int32, (CHUNK, CHUNK), 1)

    def local(c, carry):
        at = pl.ds(pl.multiple_of(c * CHUNK, CHUNK), CHUNK)
        for h in range(heads):
            lanes = slice(h * channels, (h + 1) * channels)
            queries = q_ref[at, lanes].astype(F32)
            feature = queries / (1.0 + jnp.exp(-queries))
            value_rows = v_ref[at, lanes]
            extra = extra_ref[at, h : h + 1]
            scores = jnp.zeros((CHUNK, CHUNK), F32)
            for way, (logit_ref, bound_ref) in enumerate(((ff_ref, lbf_ref), (fb_ref, lbb_ref))):
                key, decay = gates(logit_ref[at, lanes].astype(F32), bound_ref[:, lanes], extra)
                order = (rows <= cols) if way else (rows >= cols)
                total = jnp.dot(
                    order.astype(F32),
                    decay,
                    preferred_element_type=F32,
                    precision=lax.Precision.HIGHEST,
                )
                edge = total[0:1] if way else total[CHUNK - 1 : CHUNK]
                scores = scores + chunk_scores(feature, key, total, way == 1, rows, cols)
                reach_ref[way, h, c] = (feature * jnp.exp(total)).astype(BF16)
                faded = (key * jnp.exp(edge - total)).astype(BF16)
                part_ref[way, h, c] = lax.dot_general(
                    value_rows, faded, (((0,), (0,)), ((), ())), preferred_element_type=F32
                )
                fade_ref[way, h, c] = jnp.broadcast_to(jnp.exp(edge), (8, channels))
            local_ref[h, c] = jnp.dot(
                scores.astype(BF16), value_rows, preferred_element_type=F32
            )
        return carry

    lax.fori_loop(0, chunks, local, 0)
    for way in range(2):
        for h in range(heads):
            state = jnp.zeros(part_ref.shape[3:], F32)
            fade = jnp.ones((1, channels), F32)
            for c in range(chunks)[:: -1 if way else 1]:
                step = fade_ref[way, h, c, 0:1]
                state = state * step + part_ref[way, h, c]
                fade = fade * step
            state_out[way, h, : state.shape[0]] = state.astype(BF16)
            state_out[way, h, state.shape[0] :] = jnp.broadcast_to(
                fade, (DECAY_ROWS, channels)
            ).astype(BF16)

    def state_copy(target, source):
        way = jnp.where(target > me, 0, 1)
        return pltpu.make_async_remote_copy(
            src_ref=state_out.at[way],
            dst_ref=state_in.at[source],
            send_sem=state_send.at[target],
            recv_sem=state_recv.at[source],
            device_id={"ep": target},
            device_id_type=MESH,
        )

    def send(step, carry):
        state_copy(lax.rem(me + step, n), me).start()
        return carry

    def receive(step, carry):
        peer = lax.rem(me + step, n)
        copy = state_copy(peer, peer)
        copy.wait_send()
        copy.wait_recv()
        return carry

    lax.fori_loop(1, n, send, 0)
    lax.fori_loop(1, n, receive, 0)
    depth = part_ref.shape[3]
    for h in range(heads):
        for way in range(2):

            def one(hop, state, way=way, h=h):
                source = n - 1 - hop if way else hop
                step = state_in[source, h, depth : depth + DECAY_ROWS].astype(F32)[0:1]
                return state * step + state_in[source, h, :depth].astype(F32)

            ahead = n - 1 - me if way else me
            state = lax.fori_loop(0, ahead, one, jnp.zeros(part_ref.shape[3:], F32))
            for c in range(chunks)[:: -1 if way else 1]:
                local_ref[h, c] += dot_rows(reach_ref[way, h, c], state.astype(BF16))
                state = state * fade_ref[way, h, c, 0:1] + part_ref[way, h, c]
        lanes = slice(h * channels, (h + 1) * channels)
        for c in range(chunks):
            at = slice(c * CHUNK, (c + 1) * CHUNK)
            combined = local_ref[h, c]
            mean_square = jnp.mean(combined * combined, axis=-1, keepdims=True)
            gate = og_ref[at, lanes].astype(F32)
            opened = combined * lax.rsqrt(mean_square + EPS) * scale_ref[:, lanes]
            hidden_ref[at, lanes] = (opened * (gate / (1.0 + jnp.exp(-gate)))).astype(BF16)
    finish_blocks(n, slots_ref, arrived_ref, slot_send, slot_recv)


def mixer(n, queries, ff, fb, values, og, lbf, lbb, extra, scale, slots):
    row_count, width = queries.shape
    heads = extra.shape[1]
    channels = width // heads
    depth = values.shape[1] // heads
    chunks = row_count // CHUNK
    vmem = pl.BlockSpec(memory_space=pltpu.VMEM)
    state = (heads, depth + DECAY_ROWS, channels)
    return pl.pallas_call(
        functools.partial(mixer_kernel, n),
        out_shape=(
            jax.ShapeDtypeStruct(values.shape, BF16),
            jax.ShapeDtypeStruct(slots.shape, slots.dtype),
        ),
        in_specs=[vmem] * 10,
        out_specs=(vmem, vmem),
        scratch_shapes=[
            pltpu.VMEM((heads, chunks, CHUNK, depth), F32),
            pltpu.VMEM((2, heads, chunks, CHUNK, channels), BF16),
            pltpu.VMEM((2, heads, chunks, depth, channels), F32),
            pltpu.VMEM((2, heads, chunks, 8, channels), F32),
            pltpu.VMEM((2,) + state, BF16),
            pltpu.VMEM((n,) + state, BF16),
            pltpu.SemaphoreType.DMA((n,)),
            pltpu.SemaphoreType.DMA((n,)),
            pltpu.SemaphoreType.DMA((n,)),
            pltpu.SemaphoreType.DMA((n,)),
        ],
        compiler_params=pltpu.CompilerParams(
            collective_id=0, has_side_effects=True, vmem_limit_bytes=48 * 2**20
        ),
        cost_estimate=pl.CostEstimate(
            flops=4 * 10**10, bytes_accessed=6 * 2**20, transcendentals=0
        ),
        name="mix_dispatch",
    )(
        queries,
        ff,
        fb,
        values,
        og,
        lbf.reshape(1, -1),
        lbb.reshape(1, -1),
        extra,
        scale.reshape(1, -1),
        slots,
    )


def normalize(tensor, gain):
    widened_values = tensor.astype(F32)
    return (
        widened_values
        * lax.rsqrt(jnp.mean(widened_values * widened_values, axis=-1, keepdims=True) + EPS)
        * gain
    ).astype(BF16)


def shards(
    queries,
    forget_forward_logits,
    forget_backward_logits,
    values,
    output_gate_logits,
    lower_bound_forward,
    lower_bound_backward,
    extra_log_decay,
    head_norm_scale,
    output_projection,
    second_residual,
    expert_norm_scale,
    routes,
    specialist_mixing_factor,
    expert_gate_matrix,
    expert_up_matrix,
    expert_down_matrix,
):
    group_rows, width_model = second_residual.shape
    quarters = lax.axis_size("tp")
    experts = lax.axis_size("ep")
    row_count = group_rows // quarters
    slot_count = 2 * TOPK * row_count // experts
    quarter = lax.axis_index("tp")
    gate_all = lax.all_gather(expert_gate_matrix[0], "tp", axis=0)
    up_all = lax.all_gather(expert_up_matrix[0], "tp", axis=0)
    down_all = lax.all_gather(expert_down_matrix[0], "tp", axis=0, tiled=True)
    own_rows = normalize(
        lax.dynamic_slice_in_dim(second_residual, quarter * row_count, row_count, 0),
        expert_norm_scale,
    )
    flat_routes = lax.dynamic_slice_in_dim(routes, quarter * row_count, row_count, 0).reshape(-1)
    expert_hits = (flat_routes[:, None] == jnp.arange(experts, dtype=jnp.int32)[None, :]).astype(
        jnp.int32
    )
    ranking = jnp.sum(jnp.cumsum(expert_hits, axis=0) * expert_hits, axis=1) - 1
    target = flat_routes * slot_count + ranking
    own_pick = (
        target[:, None] == jnp.arange(experts * slot_count, dtype=jnp.int32)[None, :]
    ).astype(BF16)
    chooser = own_pick.reshape(row_count, TOPK, -1).sum(axis=1)
    outgoing = jnp.einsum("rs,rd->sd", chooser, own_rows, preferred_element_type=F32).astype(BF16)
    mixer_hidden, arrived = mixer(
        experts,
        queries,
        forget_forward_logits,
        forget_backward_logits,
        values,
        output_gate_logits,
        lower_bound_forward,
        lower_bound_backward,
        extra_log_decay,
        head_norm_scale,
        outgoing.reshape(experts, slot_count, width_model),
    )
    mixer_output = lax.psum_scatter(
        jnp.dot(mixer_hidden, output_projection, preferred_element_type=F32).astype(BF16),
        "tp",
        scatter_dimension=0,
        tiled=True,
    )
    rows_in = arrived.reshape(-1, width_model)
    hidden = []
    for part in range(quarters):
        gated = jnp.dot(rows_in, gate_all[part], preferred_element_type=F32)
        lifted = jnp.dot(rows_in, up_all[part], preferred_element_type=F32)
        hidden.append((jax.nn.silu(gated) * lifted).astype(BF16))
    results = jnp.dot(
        jnp.concatenate(hidden, axis=1), down_all, preferred_element_type=F32
    ).astype(BF16)
    returned = exchange(results.reshape(experts, slot_count, width_model), experts)
    gathered = jnp.dot(
        own_pick, returned.reshape(-1, width_model), preferred_element_type=F32
    )
    blended = jnp.sum(
        gathered.reshape(row_count, TOPK, width_model) * specialist_mixing_factor[:, :, None],
        axis=1,
    )
    return (mixer_output, blended.astype(BF16))


def solution(mesh):
    in_specs = (
        P("ep", "tp"),
        P("ep", "tp"),
        P("ep", "tp"),
        P("ep", "tp"),
        P("ep", "tp"),
        P("tp"),
        P("tp"),
        P("ep", "tp"),
        P("tp"),
        P("tp", None),
        P("ep", None),
        P(),
        P("ep", None),
        P(("ep", "tp"), None),
        P("ep", None, "tp"),
        P("ep", None, "tp"),
        P("ep", "tp", None),
    )
    out_specs = (P(("ep", "tp"), None), P(("ep", "tp"), None))
    return jax.shard_map(shards, mesh=mesh, in_specs=in_specs, out_specs=out_specs, check_vma=False)
```

```python
import functools

import jax
import jax.numpy as jnp
from jax import lax
from jax.experimental import pallas as pl
from jax.experimental.pallas import tpu as pltpu
from jax.sharding import PartitionSpec as P

TOPK = 2
CHUNK = 128
LEAF = 16
DECAY_ROWS = 16
EPS = 1e-06
MESH = pl.DeviceIdType.MESH
F32 = jnp.float32
BF16 = jnp.bfloat16


def neighbours():
    place, count = lax.axis_index("tp"), lax.axis_size("tp")
    return place + 1 - 2 * lax.rem(place, 2), lax.rem(place + count // 2, count)


def greet(axis, n):
    me = lax.axis_index(axis)
    barrier = pltpu.get_barrier_semaphore()

    def one(step, carry):
        peer = lax.rem(me + step, n)
        pl.semaphore_signal(barrier, inc=1, device_id={axis: peer}, device_id_type=MESH)
        return carry

    lax.fori_loop(1, n, one, 0)


def block_copy(axis, out_ref, in_ref, send_sem, recv_sem, target, source):
    return pltpu.make_async_remote_copy(
        src_ref=out_ref.at[target],
        dst_ref=in_ref.at[source],
        send_sem=send_sem.at[target],
        recv_sem=recv_sem.at[source],
        device_id={axis: target},
        device_id_type=MESH,
    )


def start_blocks(axis, n, out_ref, in_ref, send_sem, recv_sem):
    me = lax.axis_index(axis)

    def one(step, carry):
        peer = lax.rem(me + step, n)
        block_copy(axis, out_ref, in_ref, send_sem, recv_sem, peer, me).start()
        return carry

    lax.fori_loop(1, n, one, 0)
    in_ref[me] = out_ref[me]


def finish_blocks(axis, n, out_ref, in_ref, send_sem, recv_sem):
    me = lax.axis_index(axis)

    def one(step, carry):
        peer = lax.rem(me + step, n)
        copy = block_copy(axis, out_ref, in_ref, send_sem, recv_sem, peer, peer)
        copy.wait_send()
        copy.wait_recv()
        return carry

    lax.fori_loop(1, n, one, 0)


def exchange_kernel(n, quarters, rows_ref, part_ref, back_ref, sums_ref, *sems):
    greet("ep", n)
    greet("tp", quarters)
    pl.semaphore_wait(pltpu.get_barrier_semaphore(), n + quarters - 2)
    start_blocks("ep", n, rows_ref, back_ref, *sems[:2])
    start_blocks("tp", quarters, part_ref, sums_ref, *sems[2:])
    finish_blocks("tp", quarters, part_ref, sums_ref, *sems[2:])
    finish_blocks("ep", n, rows_ref, back_ref, *sems[:2])


def exchange(blocks, partials, n, quarters):
    vmem = pl.BlockSpec(memory_space=pltpu.VMEM)
    return pl.pallas_call(
        functools.partial(exchange_kernel, n, quarters),
        out_shape=(
            jax.ShapeDtypeStruct(blocks.shape, blocks.dtype),
            jax.ShapeDtypeStruct(partials.shape, partials.dtype),
        ),
        in_specs=[vmem, vmem],
        out_specs=(vmem, vmem),
        scratch_shapes=[
            pltpu.SemaphoreType.DMA((n,)),
            pltpu.SemaphoreType.DMA((n,)),
            pltpu.SemaphoreType.DMA((quarters,)),
            pltpu.SemaphoreType.DMA((quarters,)),
        ],
        compiler_params=pltpu.CompilerParams(
            collective_id=1, has_side_effects=True, vmem_limit_bytes=32 * 2**20
        ),
        cost_estimate=pl.CostEstimate(
            flops=2 * 10**10, bytes_accessed=4 * blocks.size * 2, transcendentals=0
        ),
        name="return_rows",
    )(blocks, partials)


def dot_rows(a, b):
    return lax.dot_general(a, b, (((1,), (1,)), ((), ())), preferred_element_type=F32)


def gates(logits, bound, extra):
    shrink = jnp.exp(-logits)
    opened = 1.0 / (1.0 + shrink)
    floor_part = 1.0 / (1.0 + jnp.exp(-bound))
    complement = 1.0 / (1.0 + jnp.exp(bound))
    decay = jnp.log(floor_part + complement * opened) + extra
    return complement * (shrink * opened), decay


def referenced(total, size, place):
    blocks = total.reshape(CHUNK // size, size, total.shape[-1])
    anchor = jnp.broadcast_to(blocks[:, place : place + 1, :], blocks.shape)
    return total - anchor.reshape(total.shape)


def chunk_scores(feature, key, total, backward, rows, cols):
    scores = jnp.zeros((CHUNK, CHUNK), F32)
    size = CHUNK
    while size > LEAF:
        half = size // 2
        reach = jnp.exp(-jnp.abs(referenced(total, size, half if backward else half - 1)))
        part = dot_rows((feature * reach).astype(BF16), (key * reach).astype(BF16))
        late, early = (cols, rows) if backward else (rows, cols)
        mask = (rows // size == cols // size) & (late % size >= half) & (early % size < half)
        scores = scores + jnp.where(mask, part, 0.0)
        size = half
    spread = referenced(total, LEAF, LEAF // 2 if backward else LEAF // 2 - 1)
    part = dot_rows(
        (feature * jnp.exp(spread)).astype(BF16), (key * jnp.exp(-spread)).astype(BF16)
    )
    mask = (rows // LEAF == cols // LEAF) & ((rows <= cols) if backward else (rows >= cols))
    return scores + jnp.where(mask, part, 0.0)


def mixer_kernel(
    n,
    q_ref,
    ff_ref,
    fb_ref,
    v_ref,
    og_ref,
    lbf_ref,
    lbb_ref,
    extra_ref,
    scale_ref,
    slots_ref,
    gate_ref,
    up_ref,
    down_ref,
    hidden_ref,
    arrived_ref,
    gates_ref,
    ups_ref,
    downs_ref,
    local_ref,
    reach_ref,
    part_ref,
    fade_ref,
    state_out,
    state_in,
    slot_send,
    slot_recv,
    state_send,
    state_recv,
    weight_send,
    weight_recv,
):
    me = lax.axis_index("ep")
    row_count, width = q_ref.shape
    chunks = row_count // CHUNK
    heads = extra_ref.shape[1]
    channels = width // heads
    beside, across = neighbours()
    greet("ep", n)
    barrier = pltpu.get_barrier_semaphore()
    for peer in (beside, across):
        pl.semaphore_signal(barrier, inc=1, device_id={"tp": peer}, device_id_type=MESH)
    pl.semaphore_wait(barrier, n + 1)
    weights = ((gate_ref, gates_ref), (up_ref, ups_ref), (down_ref, downs_ref))

    def weight_copy(i, hop):
        own, held = weights[i]
        return pltpu.make_async_remote_copy(
            src_ref=held.at[1] if hop == 2 else own,
            dst_ref=held.at[hop],
            send_sem=weight_send.at[i, hop],
            recv_sem=weight_recv.at[i, hop],
            device_id={"tp": across if hop == 1 else beside},
            device_id_type=MESH,
        )

    for i in range(3):
        weight_copy(i, 1).start()
    start_blocks("ep", n, slots_ref, arrived_ref, slot_send, slot_recv)
    for i in range(3):
        weight_copy(i, 0).start()
    rows = lax.broadcasted_iota(jnp.int32, (CHUNK, CHUNK), 0)
    cols = lax.broadcasted_iota(jnp.int32, (CHUNK, CHUNK), 1)

    def local(c, carry):
        at = pl.ds(pl.multiple_of(c * CHUNK, CHUNK), CHUNK)
        for h in range(heads):
            lanes = slice(h * channels, (h + 1) * channels)
            queries = q_ref[at, lanes].astype(F32)
            feature = queries / (1.0 + jnp.exp(-queries))
            value_rows = v_ref[at, lanes]
            extra = extra_ref[at, h : h + 1]
            scores = jnp.zeros((CHUNK, CHUNK), F32)
            for way, (logit_ref, bound_ref) in enumerate(((ff_ref, lbf_ref), (fb_ref, lbb_ref))):
                key, decay = gates(logit_ref[at, lanes].astype(F32), bound_ref[:, lanes], extra)
                order = (rows <= cols) if way else (rows >= cols)
                total = jnp.dot(
                    order.astype(F32),
                    decay,
                    preferred_element_type=F32,
                    precision=lax.Precision.HIGHEST,
                )
                edge = total[0:1] if way else total[CHUNK - 1 : CHUNK]
                scores = scores + chunk_scores(feature, key, total, way == 1, rows, cols)
                reach_ref[way, h, c] = (feature * jnp.exp(total)).astype(BF16)
                faded = (key * jnp.exp(edge - total)).astype(BF16)
                part_ref[way, h, c] = lax.dot_general(
                    value_rows, faded, (((0,), (0,)), ((), ())), preferred_element_type=F32
                )
                fade_ref[way, h, c] = jnp.broadcast_to(jnp.exp(edge), (8, channels))
            local_ref[h, c] = jnp.dot(
                scores.astype(BF16), value_rows, preferred_element_type=F32
            )
        return carry

    lax.fori_loop(0, chunks, local, 0)
    for way in range(2):
        for h in range(heads):
            state = jnp.zeros(part_ref.shape[3:], F32)
            fade = jnp.ones((1, channels), F32)
            for c in range(chunks)[:: -1 if way else 1]:
                step = fade_ref[way, h, c, 0:1]
                state = state * step + part_ref[way, h, c]
                fade = fade * step
            state_out[way, h, : state.shape[0]] = state.astype(BF16)
            state_out[way, h, state.shape[0] :] = jnp.broadcast_to(
                fade, (DECAY_ROWS, channels)
            ).astype(BF16)

    def state_copy(target, source):
        way = jnp.where(target > me, 0, 1)
        return pltpu.make_async_remote_copy(
            src_ref=state_out.at[way],
            dst_ref=state_in.at[source],
            send_sem=state_send.at[target],
            recv_sem=state_recv.at[source],
            device_id={"ep": target},
            device_id_type=MESH,
        )

    def send(step, carry):
        state_copy(lax.rem(me + step, n), me).start()
        return carry

    def receive(step, carry):
        peer = lax.rem(me + step, n)
        copy = state_copy(peer, peer)
        copy.wait_send()
        copy.wait_recv()
        return carry

    lax.fori_loop(1, n, send, 0)
    weight_copy(0, 1).wait_recv()
    weight_copy(0, 2).start()
    lax.fori_loop(1, n, receive, 0)
    depth = part_ref.shape[3]
    for h in range(heads):
        for way in range(2):

            def one(hop, state, way=way, h=h):
                source = n - 1 - hop if way else hop
                step = state_in[source, h, depth : depth + DECAY_ROWS].astype(F32)[0:1]
                return state * step + state_in[source, h, :depth].astype(F32)

            ahead = n - 1 - me if way else me
            state = lax.fori_loop(0, ahead, one, jnp.zeros(part_ref.shape[3:], F32))
            for c in range(chunks)[:: -1 if way else 1]:
                local_ref[h, c] += dot_rows(reach_ref[way, h, c], state.astype(BF16))
                state = state * fade_ref[way, h, c, 0:1] + part_ref[way, h, c]
        lanes = slice(h * channels, (h + 1) * channels)
        for c in range(chunks):
            at = slice(c * CHUNK, (c + 1) * CHUNK)
            combined = local_ref[h, c]
            mean_square = jnp.mean(combined * combined, axis=-1, keepdims=True)
            gate = og_ref[at, lanes].astype(F32)
            opened = combined * lax.rsqrt(mean_square + EPS) * scale_ref[:, lanes]
            hidden_ref[at, lanes] = (opened * (gate / (1.0 + jnp.exp(-gate)))).astype(BF16)
    for i in (1, 2):
        weight_copy(i, 1).wait_recv()
        weight_copy(i, 2).start()
    finish_blocks("ep", n, slots_ref, arrived_ref, slot_send, slot_recv)
    for i in range(3):
        weight_copy(i, 1).wait_send()
        for hop in (0, 2):
            weight_copy(i, hop).wait_send()
            weight_copy(i, hop).wait_recv()


def mixer(n, queries, ff, fb, values, og, lbf, lbb, extra, scale, slots, gate, up, down):
    row_count, width = queries.shape
    heads = extra.shape[1]
    channels = width // heads
    depth = values.shape[1] // heads
    chunks = row_count // CHUNK
    vmem = pl.BlockSpec(memory_space=pltpu.VMEM)
    anywhere = pl.BlockSpec(memory_space=pl.ANY)
    state = (heads, depth + DECAY_ROWS, channels)
    return pl.pallas_call(
        functools.partial(mixer_kernel, n),
        out_shape=(
            jax.ShapeDtypeStruct(values.shape, BF16),
            jax.ShapeDtypeStruct(slots.shape, slots.dtype),
        )
        + tuple(jax.ShapeDtypeStruct((3,) + w.shape, w.dtype) for w in (gate, up, down)),
        in_specs=[vmem] * 10 + [anywhere] * 3,
        out_specs=(vmem, vmem) + (anywhere,) * 3,
        scratch_shapes=[
            pltpu.VMEM((heads, chunks, CHUNK, depth), F32),
            pltpu.VMEM((2, heads, chunks, CHUNK, channels), BF16),
            pltpu.VMEM((2, heads, chunks, depth, channels), F32),
            pltpu.VMEM((2, heads, chunks, 8, channels), F32),
            pltpu.VMEM((2,) + state, BF16),
            pltpu.VMEM((n,) + state, BF16),
            pltpu.SemaphoreType.DMA((n,)),
            pltpu.SemaphoreType.DMA((n,)),
            pltpu.SemaphoreType.DMA((n,)),
            pltpu.SemaphoreType.DMA((n,)),
            pltpu.SemaphoreType.DMA((3, 3)),
            pltpu.SemaphoreType.DMA((3, 3)),
        ],
        compiler_params=pltpu.CompilerParams(
            collective_id=0, has_side_effects=True, vmem_limit_bytes=48 * 2**20
        ),
        cost_estimate=pl.CostEstimate(
            flops=4 * 10**10, bytes_accessed=6 * 2**20, transcendentals=0
        ),
        name="mix_dispatch",
    )(
        queries,
        ff,
        fb,
        values,
        og,
        lbf.reshape(1, -1),
        lbb.reshape(1, -1),
        extra,
        scale.reshape(1, -1),
        slots,
        gate,
        up,
        down,
    )


def normalize(tensor, gain):
    widened_values = tensor.astype(F32)
    return (
        widened_values
        * lax.rsqrt(jnp.mean(widened_values * widened_values, axis=-1, keepdims=True) + EPS)
        * gain
    ).astype(BF16)


def shards(
    queries,
    forget_forward_logits,
    forget_backward_logits,
    values,
    output_gate_logits,
    lower_bound_forward,
    lower_bound_backward,
    extra_log_decay,
    head_norm_scale,
    output_projection,
    second_residual,
    expert_norm_scale,
    routes,
    specialist_mixing_factor,
    expert_gate_matrix,
    expert_up_matrix,
    expert_down_matrix,
):
    group_rows, width_model = second_residual.shape
    quarters = lax.axis_size("tp")
    experts = lax.axis_size("ep")
    row_count = group_rows // quarters
    slot_count = 2 * TOPK * row_count // experts
    quarter = lax.axis_index("tp")
    gate, up, down = expert_gate_matrix[0], expert_up_matrix[0], expert_down_matrix[0]
    own_rows = normalize(
        lax.dynamic_slice_in_dim(second_residual, quarter * row_count, row_count, 0),
        expert_norm_scale,
    )
    flat_routes = lax.dynamic_slice_in_dim(routes, quarter * row_count, row_count, 0).reshape(-1)
    expert_hits = (flat_routes[:, None] == jnp.arange(experts, dtype=jnp.int32)[None, :]).astype(
        jnp.int32
    )
    ranking = jnp.sum(jnp.cumsum(expert_hits, axis=0) * expert_hits, axis=1) - 1
    target = flat_routes * slot_count + ranking
    own_pick = (
        target[:, None] == jnp.arange(experts * slot_count, dtype=jnp.int32)[None, :]
    ).astype(BF16)
    chooser = own_pick.reshape(row_count, TOPK, -1).sum(axis=1)
    outgoing = jnp.einsum("rs,rd->sd", chooser, own_rows, preferred_element_type=F32).astype(BF16)
    mixer_hidden, arrived, gates_held, ups_held, downs_held = mixer(
        experts,
        queries,
        forget_forward_logits,
        forget_backward_logits,
        values,
        output_gate_logits,
        lower_bound_forward,
        lower_bound_backward,
        extra_log_decay,
        head_norm_scale,
        outgoing.reshape(experts, slot_count, width_model),
        gate,
        up,
        down,
    )
    partials = jnp.dot(mixer_hidden, output_projection, preferred_element_type=F32).astype(BF16)
    rows_in = arrived.reshape(-1, width_model)

    def hidden_part(gate_part, up_part):
        gated = jnp.dot(rows_in, gate_part, preferred_element_type=F32)
        lifted = jnp.dot(rows_in, up_part, preferred_element_type=F32)
        return (jax.nn.silu(gated) * lifted).astype(BF16)

    result = jnp.dot(hidden_part(gate, up), down, preferred_element_type=F32)
    rest = jnp.concatenate([hidden_part(gates_held[i], ups_held[i]) for i in range(3)], axis=1)
    result = result + jnp.dot(
        rest, downs_held.reshape(-1, width_model), preferred_element_type=F32
    )
    returned, pieces = exchange(
        result.astype(BF16).reshape(experts, slot_count, width_model),
        partials.reshape(quarters, row_count, width_model),
        experts,
        quarters,
    )
    mixer_output = jnp.sum(pieces.astype(F32), axis=0).astype(BF16)
    gathered = jnp.dot(
        own_pick, returned.reshape(-1, width_model), preferred_element_type=F32
    )
    blended = jnp.sum(
        gathered.reshape(row_count, TOPK, width_model) * specialist_mixing_factor[:, :, None],
        axis=1,
    )
    return (mixer_output, blended.astype(BF16))


def solution(mesh):
    in_specs = (
        P("ep", "tp"),
        P("ep", "tp"),
        P("ep", "tp"),
        P("ep", "tp"),
        P("ep", "tp"),
        P("tp"),
        P("tp"),
        P("ep", "tp"),
        P("tp"),
        P("tp", None),
        P("ep", None),
        P(),
        P("ep", None),
        P(("ep", "tp"), None),
        P("ep", None, "tp"),
        P("ep", None, "tp"),
        P("ep", "tp", None),
    )
    out_specs = (P(("ep", "tp"), None), P(("ep", "tp"), None))
    return jax.shard_map(shards, mesh=mesh, in_specs=in_specs, out_specs=out_specs, check_vma=False)
```
